512 devices in a mesh: sp: 128 (over z, x, core), tp: 4 (over y).
Axes of the slice: x: 4, y: 4, z: 16, core: 2. Of those that a mesh axis runs over, the one named last changes fastest.
Arguments:
- tokens: bfloat16 [16384, 2048], P(('sp', 'tp')), may hold values from -6 to 6
- pre_gain: bfloat16 [2048], replicated, may hold values from 0.099609375 to 1.8984375
- w_query: bfloat16 [2048, 1024], P('sp', 'tp'), may hold values from -0.125 to 0.125
- w_key: bfloat16 [2048, 1024], P('sp', 'tp'), may hold values from -0.125 to 0.125
- w_value: bfloat16 [2048, 2048], P('sp', 'tp'), may hold values from -0.125 to 0.125
- w_igate: bfloat16 [2048, 8], replicated, may hold values from -1 to 1
- w_fgate: bfloat16 [2048, 8], replicated, may hold values from -0.125 to 0.125
- forget_bias: float32 [8], replicated, may hold values from 4 to 16
- gate_drift: float32 [16384, 8], P('sp'), may hold values from -2 to 2, as said below
- head_gain: bfloat16 [2048], replicated, may hold values from 0.099609375 to 1.8984375
- w_out: bfloat16 [2048, 2048], P('sp', 'tp'), may hold values from -0.125 to 0.125
Outputs:
- layer_out: bfloat16 [16384, 2048], P(('sp', 'tp'))
The draws below stay inside these ranges and needn't reach their ends.
Inputs may be any that keep to these rules, and one draw needn't show every extreme that they name: `gate_drift`: constant over aligned spans of 128 positions.
All inputs are finite; a program needn't handle non-finite values.
Results may differ from the reference program's by a relative error of at most 0.02.
Values may be sent and summed in bfloat16 or wider, within the bound.
No kernel may reach another device: no remote copies, remote signals or barrier semaphores. Data moves between devices by JAX's collectives and lax.ppermute only.
A program may use at most 64 MiB of HBM per device.

```python
import math
import jax
import jax.numpy as jnp
from jax import lax

D = 2048
HEADS = 8
DK = 128
DV = 256
BLOCK = 64
TOKENS = 16384
HEADS_DEV = 2
N_TP = 4


def gate_columns(key):
    return jax.random.normal(jax.random.fold_in(key, 7), (D, HEADS), jnp.float32)


def draw_w_igate(key, part):
    base_cols = gate_columns(key)
    spread_scale = 1.0
    return jnp.clip(base_cols * (spread_scale / math.sqrt(D)), -1.0, 1.0).astype(jnp.bfloat16)


def draw_tokens(key, part):
    rough_rows = jax.random.normal(jax.random.fold_in(key, 1), (TOKENS, D), jnp.float32)
    return jnp.clip(rough_rows, -6.0, 6.0).astype(jnp.bfloat16)


def draw_forget_bias(key, part):
    head_order = jax.random.permutation(jax.random.fold_in(key, 4), HEADS)
    slow_count = HEADS // 2
    slow_heads = head_order < slow_count
    jitter = jax.random.uniform(jax.random.fold_in(key, 5), (HEADS,), jnp.float32, -0.3, 0.3)
    return jnp.where(slow_heads, math.log(TOKENS) + 0.8, math.log(100.0)) + jitter


def draw_gate_drift(key, part):
    span_count = TOKENS // (2 * BLOCK)
    span_level = jax.random.uniform(jax.random.fold_in(key, 6), (span_count, HEADS), jnp.float32, -1.5, 1.5)
    return jnp.repeat(span_level, 2 * BLOCK, axis=0)


def block_scale(key, shape, shards, low, high):
    def one(position, blocks):
        heights = jax.random.uniform(jax.random.fold_in(jax.random.fold_in(key, 6), position), (blocks,), jnp.float32, low / len(shards), high / len(shards))
        return jnp.repeat(jnp.exp(heights), shape[position] // blocks).reshape((-1,) + (1,) * (len(shape) - position - 1))

    level = one(*shards[0])
    for cut in shards[1:]:
        level = level * one(*cut)
    return level


def noise(stream_key, extent, spread, most, cuts=(), dtype=jnp.bfloat16):
    factor_of = block_scale(stream_key, extent, cuts, -0.22, 0.18) if cuts else 1.0
    entries = jax.random.normal(stream_key, extent, jnp.float32) * spread * factor_of
    return jnp.minimum(jnp.maximum(entries, -most), most).astype(dtype)


def setup_inputs(seed: int = 0) -> dict:
    streams_of = jax.random.split(jax.random.key(seed), 12)
    tokens = draw_tokens(jax.random.fold_in(streams_of[11], 71), 0)
    pre_gain = jnp.clip(1.0 + 0.18 * jax.random.normal(streams_of[1], (D,), jnp.float32), 0.099609375, 1.8984375).astype(jnp.bfloat16)
    w_query = noise(streams_of[2], (D, HEADS * DK), D ** -0.5, 0.125, ((0, 128), (1, 4)))
    w_key = noise(streams_of[3], (D, HEADS * DK), D ** -0.5, 0.125, ((0, 128), (1, 4)))
    w_value = noise(streams_of[4], (D, HEADS * DV), D ** -0.5, 0.125, ((0, 128), (1, 4)))
    w_igate = draw_w_igate(jax.random.fold_in(streams_of[11], 71), 0)
    w_fgate = noise(streams_of[6], (D, HEADS), D ** -0.5, 0.125)
    forget_bias = draw_forget_bias(jax.random.fold_in(streams_of[11], 71), 0)
    gate_drift = draw_gate_drift(jax.random.fold_in(streams_of[11], 71), 0)
    head_gain = jnp.clip(1.0 + 0.18 * jax.random.normal(streams_of[9], (HEADS * DV,), jnp.float32), 0.099609375, 1.8984375).astype(jnp.bfloat16)
    w_out = noise(streams_of[10], (D, HEADS * DV), (HEADS * DV) ** -0.5, 0.125, ((0, 128), (1, 4)))
    return dict(tokens=tokens, pre_gain=pre_gain, w_query=w_query, w_key=w_key, w_value=w_value, w_igate=w_igate, w_fgate=w_fgate, forget_bias=forget_bias, gate_drift=gate_drift, head_gain=head_gain, w_out=w_out)


norm_floor = 0.1
lowest_log = -1e+30
highest = lax.Precision.HIGHEST

def advance(memory, summary):
    old_mat, old_vec, old_top = memory
    span_log, span_top, span_mat, span_vec = summary
    new_top = jnp.maximum(span_log + old_top, span_top)
    kept_part = jnp.exp(span_log + old_top - new_top)
    fresh_part = jnp.exp(span_top - new_top)
    return (kept_part[:, None, None] * old_mat + fresh_part[:, None, None] * span_mat, kept_part[:, None] * old_vec + fresh_part[:, None] * span_vec, new_top)

def blend_parts(first_part, second_part):
    numer_first, denom_first, peak_first = first_part
    numer_second, denom_second, peak_second = second_part
    new_top = jnp.maximum(peak_first, peak_second)
    weight_first = jnp.exp(peak_first - new_top)
    weight_second = jnp.exp(peak_second - new_top)
    return (weight_first[..., None] * numer_first + weight_second[..., None] * numer_second, weight_first * denom_first + weight_second * denom_second, new_top)

def reference(tokens, pre_gain, w_query, w_key, w_value, w_igate, w_fgate, forget_bias, gate_drift, head_gain, w_out):
    token_wide = tokens.astype(jnp.float32)
    scaled = token_wide * lax.rsqrt(lax.optimization_barrier(jnp.mean(token_wide * token_wide, axis=1, keepdims=True)) + norm_floor)
    normed = (scaled * pre_gain.astype(jnp.float32)).astype(jnp.bfloat16)
    queries = jnp.dot(normed, w_query, preferred_element_type=jnp.float32).astype(jnp.bfloat16)
    keys_all = (jnp.dot(normed, w_key, preferred_element_type=jnp.float32) * DK ** (-0.5)).astype(jnp.bfloat16)
    values_all = jnp.dot(normed, w_value, preferred_element_type=jnp.float32).astype(jnp.bfloat16)
    log_input = jnp.dot(normed, w_igate, preferred_element_type=jnp.float32)
    forget_pre = jnp.dot(normed, w_fgate, preferred_element_type=jnp.float32) + forget_bias
    log_forget = jax.nn.log_sigmoid(forget_pre + gate_drift)
    blocks = TOKENS // BLOCK
    head_gains = head_gain.astype(jnp.float32).reshape(HEADS, DV)
    causal = jnp.arange(BLOCK)[:, None] >= jnp.arange(BLOCK)[None, :]

    def block_step(carry_state, inputs):
        memory_mat, memory_vec, memory_top = carry_state
        query_blk, key_blk, value_blk, input_row, forget_row = inputs
        query_wide = query_blk.astype(jnp.float32)
        key_wide = key_blk.astype(jnp.float32)
        value_wide = value_blk.astype(jnp.float32)
        input_gate = input_row.T
        forget_gate = forget_row.T
        within = jnp.cumsum(forget_gate, axis=1)
        log_pair = jnp.where(causal, within[:, :, None] - within[:, None, :] + input_gate[:, None, :], -jnp.inf)
        peak_intra = lax.optimization_barrier(jnp.max(log_pair, axis=2))
        scores = jnp.einsum('shd,rhd->hsr', query_wide, key_wide, precision=highest)
        weights = scores * jnp.exp(log_pair - peak_intra[:, :, None])
        weights_low = lax.optimization_barrier(weights.astype(jnp.bfloat16))
        numer_intra = jnp.einsum('hsr,rhv->hsv', weights_low.astype(jnp.float32), value_wide, precision=highest)
        denom_intra = lax.optimization_barrier(jnp.sum(weights, axis=2))
        carried_log = within + memory_top[:, None]
        numer_carry = jnp.einsum('hvd,shd->hsv', memory_mat, query_wide, precision=highest)
        denom_carry = jnp.einsum('hd,shd->hs', memory_vec, query_wide, precision=highest)
        numerator, denominator, peak_log = blend_parts((numer_carry, denom_carry, carried_log), (numer_intra, denom_intra, peak_intra))
        hidden = numerator / jnp.maximum(jnp.abs(denominator), jnp.exp(-peak_log))[:, :, None]
        hidden = hidden.transpose(1, 0, 2)
        normed_heads = hidden * lax.rsqrt(lax.optimization_barrier(jnp.mean(hidden * hidden, axis=2, keepdims=True)) + norm_floor) * head_gains
        span_log = within[:, -1]
        log_write = span_log[:, None] - within + input_gate
        span_top = lax.optimization_barrier(jnp.max(log_write, axis=1))
        write_scale = jnp.exp(log_write - span_top[:, None])
        key_scaled = key_wide * write_scale.T[:, :, None]
        span_mat = jnp.einsum('rhv,rhd->hvd', value_wide, key_scaled, precision=highest)
        span_vec = lax.optimization_barrier(jnp.sum(key_scaled, axis=0))
        new_state = advance(carry_state, (span_log, span_top, span_mat, span_vec))
        return (new_state, normed_heads.astype(jnp.bfloat16).reshape(BLOCK, HEADS * DV))
    init_state = (jnp.zeros((HEADS, DV, DK), jnp.float32), jnp.zeros((HEADS, DK), jnp.float32), jnp.full((HEADS,), lowest_log, jnp.float32))
    scanned = (queries.reshape(blocks, BLOCK, HEADS, DK), keys_all.reshape(blocks, BLOCK, HEADS, DK), values_all.reshape(blocks, BLOCK, HEADS, DV), log_input.reshape(blocks, BLOCK, HEADS), log_forget.reshape(blocks, BLOCK, HEADS))
    outputs = lax.scan(block_step, init_state, scanned)[1]
    normed_all = outputs.reshape(TOKENS, HEADS * DV)
    group_width = HEADS_DEV * DV
    total_sum = jnp.zeros((TOKENS, D), jnp.float32)
    for group_index in range(N_TP):
        columns = slice(group_index * group_width, (group_index + 1) * group_width)
        partial_value = lax.dot_general(normed_all[:, columns], w_out[:, columns], (((1,), (1,)), ((), ())), preferred_element_type=jnp.float32)
        partial_value = lax.optimization_barrier(partial_value.astype(jnp.bfloat16))
        total_sum = total_sum + partial_value.astype(jnp.float32)
    return total_sum.astype(jnp.bfloat16)
```

```python
import jax
import jax.numpy as jnp
from jax import lax
from jax.experimental import pallas as pl
from jax.experimental.pallas import tpu as pltpu
from jax.sharding import Mesh
from jax.sharding import PartitionSpec as P

SP = ("z", "x", "c")
SP_TP = ("z", "x", "c", "y")
ROWS = ("z", "x")
HEADS = 8
DK = 128
DV = 256
norm_floor = 0.1
lowest_log = -1e30
highest = lax.Precision.HIGHEST
f32 = jnp.float32
bf16 = jnp.bfloat16


def lane_ids(shape):
    return lax.broadcasted_iota(jnp.int32, shape, 1)


def row_ids(shape):
    return lax.broadcasted_iota(jnp.int32, shape, 0)


def prepare_kernel(tokens_ref, gain_ref, gate_w_ref, offset_ref, out_ref):
    wide = tokens_ref[...].astype(f32)
    scaled = wide * lax.rsqrt(jnp.mean(wide * wide, axis=1, keepdims=True) + norm_floor)
    normed = (scaled * gain_ref[...].astype(f32)).astype(bf16)
    width = normed.shape[1]
    out_ref[:, :width] = normed
    gates = jnp.dot(normed, gate_w_ref[...], preferred_element_type=f32)
    forget = gates + offset_ref[...]
    log_forget = jnp.minimum(forget, 0.0) - jnp.log1p(jnp.exp(-jnp.abs(forget)))
    lane = lane_ids(gates.shape)
    value = jnp.where(lane % 16 < 8, gates, log_forget)
    high = value.astype(bf16).astype(f32)
    middle = (value - high).astype(bf16).astype(f32)
    low = value - high - middle
    piece = jnp.where(lane < 16, high, jnp.where(lane < 32, middle, low))
    out_ref[:, width:] = jnp.where(lane < 48, piece, 0.0).astype(bf16)


def cell_kernel(head_ref, rows_ref, w_ref, query_ref, message_ref, numer_ref, aux_ref):
    head = head_ref[0]
    length = rows_ref.shape[0]
    width = rows_ref.shape[1] - 128
    x_size = w_ref.shape[0]
    run = width // (x_size * (w_ref.shape[1] // 32))
    total = jnp.zeros((length, w_ref.shape[2]), f32)
    for k in range(width // 256):
        parts = [
            w_ref[x, z * run : (z + 1) * run, :] for z in (2 * k, 2 * k + 1) for x in range(x_size)
        ]
        total = total + jnp.dot(
            rows_ref[:, k * 256 : (k + 1) * 256],
            jnp.concatenate(parts, axis=0),
            preferred_element_type=f32,
        )
    query = total[:, :DK].astype(bf16)
    key = (total[:, DK : 2 * DK] * (DK**-0.5)).astype(bf16)
    value = total[:, 2 * DK :].astype(bf16)
    query_ref[...] = query

    gates = rows_ref[:, width:].astype(f32)
    lane = lane_ids(gates.shape)
    input_col = jnp.sum(jnp.where(lane % 16 == head, gates, 0.0), axis=1, keepdims=True)
    forget_col = jnp.sum(jnp.where(lane % 16 == head + 8, gates, 0.0), axis=1, keepdims=True)
    both = jnp.where(lane == 0, input_col, jnp.where(lane == 1, forget_col, 0.0))
    both_rows = both.T
    input_row = both_rows[0:1, :]
    forget_row = both_rows[1:2, :]

    square = (length, length)
    s_id = row_ids(square)
    r_id = lane_ids(square)
    up_to = jnp.where(r_id <= s_id, forget_row, 0.0)
    after = jnp.where(s_id > r_id, 1.0, 0.0).astype(f32)
    decay = jnp.dot(up_to, after, precision=highest, preferred_element_type=f32)
    within = jnp.sum(up_to, axis=1, keepdims=True)
    suffix = jnp.sum(jnp.where(r_id > s_id, forget_row, 0.0), axis=1, keepdims=True)
    causal = r_id <= s_id
    log_pair = jnp.where(causal, decay + input_row, lowest_log)
    peak = jnp.max(log_pair, axis=1, keepdims=True)
    scores = lax.dot_general(query, key, (((1,), (1,)), ((), ())), preferred_element_type=f32)
    weights = jnp.where(causal, scores * jnp.exp(log_pair - peak), 0.0)
    numer_ref[...] = jnp.dot(weights.astype(bf16), value, preferred_element_type=f32)
    denom = jnp.sum(weights, axis=1, keepdims=True)
    aux_ref[...] = jnp.where(
        lane == 0, denom, jnp.where(lane == 1, peak, jnp.where(lane == 2, within, 0.0))
    )

    log_write = suffix + input_col
    top = jnp.max(log_write, axis=0, keepdims=True)
    scaled_key = key.astype(f32) * jnp.exp(log_write - top)
    state = jnp.dot(value.astype(f32).T, scaled_key, precision=highest, preferred_element_type=f32)
    vector = jnp.sum(scaled_key, axis=0, keepdims=True)
    span_log = jnp.sum(forget_row, axis=1, keepdims=True)
    peers = message_ref.shape[0] // 8
    for r in range(DV // peers):
        message_ref[pl.ds(r, peers, stride=8), :] = state[r * peers : (r + 1) * peers, :]
    small = lane_ids((peers, DK))
    message_ref[pl.ds(4, peers, stride=8), :] = jnp.broadcast_to(vector, (peers, DK))
    message_ref[pl.ds(5, peers, stride=8), :] = jnp.where(
        small == 0, span_log, jnp.where(small == 1, top, 0.0)
    )
    for r in (6, 7):
        message_ref[pl.ds(r, peers, stride=8), :] = jnp.zeros((peers, DK), f32)


def prefix_kernel(place_ref, arrived_ref, out_ref, entry_ref):
    place = place_ref[0]
    peers = arrived_ref.shape[0] // 8
    vectors = arrived_ref[pl.ds(4, peers, stride=8), :]
    facts = arrived_ref[pl.ds(5, peers, stride=8), :]
    fact_rows = facts.T
    log_row = fact_rows[0:1, :]
    top_row = fact_rows[1:2, :]
    square = (peers, peers)
    i_id = row_ids(square)
    j_id = lane_ids(square)
    before = jnp.where(j_id < i_id, log_row, 0.0)
    after = jnp.where(i_id > j_id, 1.0, 0.0).astype(f32)
    logs = jnp.dot(before, after, precision=highest, preferred_element_type=f32) + top_row
    earlier = j_id < i_id
    logs = jnp.where(earlier, logs, lowest_log)
    top = jnp.max(logs, axis=1, keepdims=True)
    mix = jnp.where(earlier, jnp.exp(logs - top), 0.0)
    count = out_ref.shape[0] // peers
    for r in range(count):
        out_ref[pl.ds(r, peers, stride=count), :] = jnp.dot(
            mix,
            arrived_ref[pl.ds(r, peers, stride=8), :],
            precision=highest,
            preferred_element_type=f32,
        )
    entries = jnp.dot(mix, vectors, precision=highest, preferred_element_type=f32)
    mine = row_ids(entries.shape) == place
    vector = jnp.sum(jnp.where(mine, entries, 0.0), axis=0, keepdims=True)
    entry_top = jnp.sum(jnp.where(mine, top, 0.0), axis=0, keepdims=True)
    row = row_ids(entry_ref.shape)
    entry_ref[...] = jnp.where(row == 0, vector, jnp.where(row == 1, entry_top, 0.0))


def finish_kernel(
    head_ref, query_ref, numer_ref, aux_ref, state_ref, entry_ref, gain_ref, w_ref, out_ref
):
    head = head_ref[0]
    count = DV * DK // (state_ref.shape[1] * 64)
    peers = state_ref.shape[0] // count
    state = jnp.concatenate(
        [state_ref[pl.ds(r, peers, stride=count), :] for r in range(count)], axis=0
    )
    query = query_ref[...].astype(f32)
    left = lax.dot_general(
        query, state, (((1,), (1,)), ((), ())), precision=highest, preferred_element_type=f32
    )
    entry_vec = entry_ref[0:1, :]
    entry_top = entry_ref[1:2, 0:1]
    left_denom = jnp.sum(query * entry_vec, axis=1, keepdims=True)
    aux = aux_ref[...]
    lane = lane_ids(aux.shape)
    denom = jnp.sum(jnp.where(lane == 0, aux, 0.0), axis=1, keepdims=True)
    peak = jnp.sum(jnp.where(lane == 1, aux, 0.0), axis=1, keepdims=True)
    within = jnp.sum(jnp.where(lane == 2, aux, 0.0), axis=1, keepdims=True)
    carried = within + entry_top
    top = jnp.maximum(peak, carried)
    own = jnp.exp(peak - top)
    old = jnp.exp(carried - top)
    numer = own * numer_ref[...] + old * left
    denom = own * denom + old * left_denom
    hidden = numer / jnp.maximum(jnp.abs(denom), jnp.exp(-top))
    gains = gain_ref[...].astype(f32)
    gain = jnp.sum(jnp.where(row_ids(gains.shape) == head, gains, 0.0), axis=0, keepdims=True)
    scale = lax.rsqrt(jnp.mean(hidden * hidden, axis=1, keepdims=True) + norm_floor)
    heads_out = (hidden * scale * gain).astype(bf16)
    x_size = w_ref.shape[0]
    run = 32
    for k in range(out_ref.shape[1] // 256):
        parts = [
            w_ref[x, z * run : (z + 1) * run, :] for z in (2 * k, 2 * k + 1) for x in range(x_size)
        ]
        out_ref[:, k * 256 : (k + 1) * 256] = lax.dot_general(
            heads_out,
            jnp.concatenate(parts, axis=0),
            (((1,), (1,)), ((), ())),
            preferred_element_type=f32,
        ).astype(bf16)


def on_device(
    tokens,
    pre_gain,
    w_query,
    w_key,
    w_value,
    w_igate,
    w_fgate,
    forget_bias,
    gate_drift,
    head_gain,
    w_out,
):
    width = tokens.shape[1]
    z_size, x_size = lax.axis_size("z"), lax.axis_size("x")
    peers = z_size * x_size
    head = (lax.axis_index("y") * 2 + lax.axis_index("c")).astype(jnp.int32).reshape(1)
    place = (lax.axis_index("z") * x_size + lax.axis_index("x")).astype(jnp.int32).reshape(1)
    smem = pl.BlockSpec(memory_space=pltpu.SMEM)
    vmem = pl.BlockSpec(memory_space=pltpu.VMEM)

    gate_w = jnp.concatenate([w_igate, w_fgate] * 3 + [jnp.zeros((width, 80), bf16)], axis=1)
    offsets = jnp.concatenate([jnp.zeros((8,), f32), forget_bias + gate_drift[0]] * 3)
    offsets = jnp.pad(offsets, (0, 80)).reshape(1, 128)
    rows = tokens.shape[0]
    own_rows = pl.pallas_call(
        prepare_kernel,
        out_shape=jax.ShapeDtypeStruct((rows, width + 128), bf16),
        in_specs=[vmem] * 4,
        out_specs=vmem,
        name="prepare",
    )(tokens, pre_gain.reshape(1, width), gate_w, offsets)
    all_rows = lax.all_gather(own_rows, ("c", "y"), axis=0, tiled=True)

    pair = jnp.stack(
        [
            jnp.concatenate(
                [
                    w_query[:, c * DK : (c + 1) * DK],
                    w_key[:, c * DK : (c + 1) * DK],
                    w_value[:, c * DV : (c + 1) * DV],
                    w_out[:, c * DV : (c + 1) * DV],
                ],
                axis=1,
            )
            for c in range(2)
        ]
    )
    mine = lax.all_to_all(pair, "c", split_axis=0, concat_axis=0, tiled=True)
    mine = mine.reshape(-1, mine.shape[2])
    along_z = lax.all_gather(mine, "z", axis=0, tiled=True)
    cut = 2 * DK + DV
    out_part = along_z[:, cut:]
    in_part = along_z[:, :cut]
    w_in = lax.all_to_all(
        jnp.broadcast_to(in_part[None], (x_size,) + in_part.shape),
        "x",
        split_axis=0,
        concat_axis=0,
        tiled=True,
    )
    w_back = lax.all_gather(out_part, "x", axis=0, tiled=False)

    length = all_rows.shape[0]
    query, message, numer, aux = pl.pallas_call(
        cell_kernel,
        out_shape=(
            jax.ShapeDtypeStruct((length, DK), bf16),
            jax.ShapeDtypeStruct((peers * 8, DK), f32),
            jax.ShapeDtypeStruct((length, DV), f32),
            jax.ShapeDtypeStruct((length, 128), f32),
        ),
        in_specs=[smem, vmem, vmem],
        out_specs=(vmem,) * 4,
        name="cell",
    )(head, all_rows, w_in)
    arrived = lax.all_to_all(message, ROWS, split_axis=0, concat_axis=0, tiled=True)
    slices, entry = pl.pallas_call(
        prefix_kernel,
        out_shape=(
            jax.ShapeDtypeStruct((DV, DK), f32),
            jax.ShapeDtypeStruct((8, 128), f32),
        ),
        in_specs=[smem, vmem],
        out_specs=(vmem,) * 2,
        name="prefix",
    )(place, arrived)
    state = lax.all_to_all(slices, ROWS, split_axis=0, concat_axis=0, tiled=True)
    partial = pl.pallas_call(
        finish_kernel,
        out_shape=jax.ShapeDtypeStruct((length, width), bf16),
        in_specs=[smem] + [vmem] * 7,
        out_specs=vmem,
        name="finish",
    )(head, query, numer, aux, state, entry, head_gain.reshape(HEADS, DV), w_back)
    pieces = lax.all_to_all(
        partial.reshape(-1, rows, width), ("c", "y"), split_axis=0, concat_axis=0, tiled=True
    )
    return pieces.astype(f32).sum(axis=0).astype(bf16)


def solution(mesh):
    split = Mesh(mesh.devices.reshape(16, 4, 2, mesh.shape["tp"]), ("z", "x", "c", "y"))
    return jax.shard_map(
        on_device,
        mesh=split,
        in_specs=(
            P(SP_TP, None),
            P(),
            P(SP, "y"),
            P(SP, "y"),
            P(SP, "y"),
            P(),
            P(),
            P(),
            P(SP, None),
            P(),
            P(SP, "y"),
        ),
        out_specs=P(SP_TP, None),
        check_vma=False,
    )
```

```python
import jax
import jax.numpy as jnp
from jax import lax
from jax.experimental import pallas as pl
from jax.experimental.pallas import tpu as pltpu
from jax.sharding import Mesh
from jax.sharding import PartitionSpec as P

SP = ("z", "x", "c")
SP_TP = ("z", "x", "c", "y")
ROWS = ("z", "x")
HEADS = 8
DK = 128
DV = 256
norm_floor = 0.1
lowest_log = -1e30
highest = lax.Precision.HIGHEST
f32 = jnp.float32
bf16 = jnp.bfloat16


def near(array):
    return pltpu.with_memory_space_constraint(array, pltpu.VMEM)


def lane_ids(shape):
    return lax.broadcasted_iota(jnp.int32, shape, 1)


def row_ids(shape):
    return lax.broadcasted_iota(jnp.int32, shape, 0)


def three_parts(value):
    high = value.astype(bf16).astype(f32)
    middle = (value - high).astype(bf16).astype(f32)
    return high, middle, value - high - middle


def prepare_kernel(bias_ref, tokens_ref, gain_ref, w_igate_ref, w_fgate_ref, drift_ref, out_ref):
    wide = tokens_ref[...].astype(f32)
    scale = lax.rsqrt(jnp.mean(wide * wide, axis=1, keepdims=True) + norm_floor)
    gain = gain_ref[...].astype(f32)
    blocks = gain.shape[0]
    normed = jnp.concatenate(
        [
            (wide[:, k * 128 : (k + 1) * 128] * scale * gain[k : k + 1, :]).astype(bf16)
            for k in range(blocks)
        ],
        axis=1,
    )
    width = normed.shape[1]
    across = (((1,), (1,)), ((), ()))
    gate_in = lax.dot_general(w_igate_ref[...], normed, across, preferred_element_type=f32)
    forget = lax.dot_general(w_fgate_ref[...], normed, across, preferred_element_type=f32)
    heads = forget.shape[0]
    line = row_ids((heads, 1))
    bias = jnp.zeros((heads, 1), f32)
    for h in range(heads):
        bias = jnp.where(line == h, bias_ref[h], bias)
    forget = forget + bias + drift_ref[:, 0:1]
    log_forget = jnp.minimum(forget, 0.0) - jnp.log1p(jnp.exp(-jnp.abs(forget)))
    lane = lane_ids((heads, 128))
    row = row_ids((heads, 128))
    place_in = jnp.where(lane % 16 == row, 1.0, 0.0).astype(f32)
    place_forget = jnp.where(lane % 16 == row + heads, 1.0, 0.0).astype(f32)
    value = jnp.dot(
        gate_in.T, place_in, precision=highest, preferred_element_type=f32
    ) + jnp.dot(log_forget.T, place_forget, precision=highest, preferred_element_type=f32)
    high, middle, low = three_parts(value)
    lane = lane_ids(value.shape)
    piece = jnp.where(lane < 16, high, jnp.where(lane < 32, middle, low))
    piece = jnp.where(lane < 48, piece, 0.0).astype(bf16)
    for k in range(out_ref.shape[0]):
        out_ref[k, :, :width] = normed
        out_ref[k, :, width:] = piece


def gates_kernel(head_ref, rows_ref, pair_ref, aux_ref, facts_ref):
    head = head_ref[0]
    gates = rows_ref[:, -128:].astype(f32)
    length = gates.shape[0]
    lane = lane_ids(gates.shape)
    input_col = jnp.sum(jnp.where(lane % 16 == head, gates, 0.0), axis=1, keepdims=True)
    forget_col = jnp.sum(jnp.where(lane % 16 == head + 8, gates, 0.0), axis=1, keepdims=True)
    both = jnp.where(lane == 0, input_col, jnp.where(lane == 1, forget_col, 0.0))
    both_rows = both.T
    input_row = both_rows[0:1, :]
    forget_row = both_rows[1:2, :]
    square = (length, length)
    s_id = row_ids(square)
    r_id = lane_ids(square)
    causal = r_id <= s_id
    up_to = jnp.where(causal, forget_row, 0.0)
    after = jnp.where(s_id > r_id, 1.0, 0.0).astype(f32)
    decay = jnp.dot(up_to, after, precision=highest, preferred_element_type=f32)
    within = jnp.sum(up_to, axis=1, keepdims=True)
    suffix = jnp.sum(jnp.where(r_id > s_id, forget_row, 0.0), axis=1, keepdims=True)
    log_pair = jnp.where(causal, decay + input_row, lowest_log)
    peak = jnp.max(log_pair, axis=1, keepdims=True)
    pair_ref[...] = jnp.where(causal, jnp.exp(log_pair - peak), 0.0)
    log_write = suffix + input_col
    top = jnp.max(log_write, axis=0, keepdims=True)
    write = jnp.exp(log_write - top)
    aux_ref[...] = jnp.where(
        lane == 1, peak, jnp.where(lane == 2, within, jnp.where(lane == 3, write, 0.0))
    )
    span_log = jnp.sum(forget_row, axis=1, keepdims=True)
    small = lane_ids(facts_ref.shape)
    facts = jnp.zeros(facts_ref.shape, f32)
    for k, piece in enumerate(three_parts(span_log) + three_parts(top)):
        facts = jnp.where(small == k, piece, facts)
    facts_ref[...] = facts


def column_of(aux, k):
    return jnp.sum(jnp.where(lane_ids(aux.shape) == k, aux, 0.0), axis=1, keepdims=True)


def state_kernel(
    rows_ref, w_ref, aux_ref, facts_ref, query_ref, key_ref, value_ref, message_ref, buffer_ref
):
    length, width = rows_ref.shape[0], rows_ref.shape[1] - 128
    x_size = w_ref.shape[0]
    run = 32
    total = jnp.zeros((length, w_ref.shape[2]), f32)
    for k in range(width // 256):
        parts = [
            w_ref[x, z * run : (z + 1) * run, :] for z in (2 * k, 2 * k + 1) for x in range(x_size)
        ]
        total = total + jnp.dot(
            rows_ref[:, k * 256 : (k + 1) * 256],
            jnp.concatenate(parts, axis=0),
            preferred_element_type=f32,
        )
    query_ref[...] = total[:, :DK].astype(bf16)
    key = (total[:, DK : 2 * DK] * (DK**-0.5)).astype(bf16)
    value = total[:, 2 * DK :].astype(bf16)
    key_ref[...] = key
    value_ref[...] = value
    scaled_key = key.astype(f32) * column_of(aux_ref[...], 3)
    state = jnp.dot(value.astype(f32).T, scaled_key, precision=highest, preferred_element_type=f32)
    vector = jnp.sum(scaled_key, axis=0, keepdims=True)
    peers = buffer_ref.shape[0] // 8
    for r in range(DV // peers):
        buffer_ref[pl.ds(r, peers, stride=8), :] = state[r * peers : (r + 1) * peers, :]
    buffer_ref[pl.ds(4, peers, stride=8), :] = jnp.broadcast_to(vector, (peers, DK))
    buffer_ref[pl.ds(5, peers, stride=8), :] = jnp.broadcast_to(facts_ref[0:1, :], (peers, DK))
    for r in (6, 7):
        buffer_ref[pl.ds(r, peers, stride=8), :] = jnp.zeros((peers, DK), f32)
    message_ref[...] = buffer_ref[...].astype(bf16)


def intra_kernel(query_ref, key_ref, value_ref, pair_ref, numer_ref, denom_ref):
    scores = lax.dot_general(
        query_ref[...], key_ref[...], (((1,), (1,)), ((), ())), preferred_element_type=f32
    )
    weights = scores * pair_ref[...]
    numer_ref[...] = jnp.dot(weights.astype(bf16), value_ref[...], preferred_element_type=f32)
    denom = jnp.sum(weights, axis=1, keepdims=True)
    denom_ref[...] = jnp.broadcast_to(denom, denom_ref.shape)


def prefix_kernel(place_ref, arrived_ref, out_ref, entry_ref, buffer_ref):
    place = place_ref[0]
    buffer_ref[...] = arrived_ref[...].astype(f32)
    peers = buffer_ref.shape[0] // 8
    vectors = buffer_ref[pl.ds(4, peers, stride=8), :]
    fact_rows = buffer_ref[pl.ds(5, peers, stride=8), :].T
    log_row = fact_rows[0:1, :] + fact_rows[1:2, :] + fact_rows[2:3, :]
    top_row = fact_rows[3:4, :] + fact_rows[4:5, :] + fact_rows[5:6, :]
    square = (peers, peers)
    i_id = row_ids(square)
    j_id = lane_ids(square)
    earlier = j_id < i_id
    before = jnp.where(earlier, log_row, 0.0)
    after = jnp.where(i_id > j_id, 1.0, 0.0).astype(f32)
    logs = jnp.dot(before, after, precision=highest, preferred_element_type=f32) + top_row
    logs = jnp.where(earlier, logs, lowest_log)
    top = jnp.max(logs, axis=1, keepdims=True)
    mix = jnp.where(earlier, jnp.exp(logs - top), 0.0)
    count = out_ref.shape[0] // peers
    for r in range(count):
        out_ref[pl.ds(r, peers, stride=count), :] = jnp.dot(
            mix,
            buffer_ref[pl.ds(r, peers, stride=8), :],
            precision=highest,
            preferred_element_type=f32,
        )
    entries = jnp.dot(mix, vectors, precision=highest, preferred_element_type=f32)
    mine = row_ids(entries.shape) == place
    vector = jnp.sum(jnp.where(mine, entries, 0.0), axis=0, keepdims=True)
    entry_top = jnp.sum(jnp.where(mine, top, 0.0), axis=0, keepdims=True)
    row = row_ids(entry_ref.shape)
    entry_ref[...] = jnp.where(row == 0, vector, jnp.where(row == 1, entry_top, 0.0))


def finish_kernel(
    head_ref,
    query_ref,
    numer_ref,
    denom_ref,
    aux_ref,
    state_ref,
    entry_ref,
    gain_ref,
    w_0_ref,
    w_1_ref,
    w_2_ref,
    w_3_ref,
    out_ref,
    w_ref,
):
    head = head_ref[0]
    my_x = head_ref[1]
    for d, piece_ref in enumerate((w_0_ref, w_1_ref, w_2_ref, w_3_ref)):
        w_ref[(my_x + 4 - d) % 4] = piece_ref[...]
    peers = 64
    count = state_ref.shape[0] // peers
    state = jnp.concatenate(
        [state_ref[pl.ds(r, peers, stride=count), :] for r in range(count)], axis=0
    )
    query = query_ref[...].astype(f32)
    left = lax.dot_general(
        query, state, (((1,), (1,)), ((), ())), precision=highest, preferred_element_type=f32
    )
    entry_vec = entry_ref[0:1, :]
    entry_top = entry_ref[1:2, 0:1]
    left_denom = jnp.sum(query * entry_vec, axis=1, keepdims=True)
    aux = aux_ref[...]
    denom = denom_ref[:, 0:1]
    peak = column_of(aux, 1)
    carried = column_of(aux, 2) + entry_top
    top = jnp.maximum(peak, carried)
    own = jnp.exp(peak - top)
    old = jnp.exp(carried - top)
    numer = own * numer_ref[...] + old * left
    denom = own * denom + old * left_denom
    hidden = numer / jnp.maximum(jnp.abs(denom), jnp.exp(-top))
    gains = gain_ref[...].astype(f32)
    row = row_ids(gains.shape)
    gain = jnp.concatenate(
        [
            jnp.sum(jnp.where(row == 2 * head + k, gains, 0.0), axis=0, keepdims=True)
            for k in range(2)
        ],
        axis=1,
    )
    scale = lax.rsqrt(jnp.mean(hidden * hidden, axis=1, keepdims=True) + norm_floor)
    heads_out = (hidden * scale * gain).astype(bf16)
    x_size = w_ref.shape[0]
    run = 32
    for k in range(out_ref.shape[1] // 256):
        parts = [
            w_ref[x, z * run : (z + 1) * run, :] for z in (2 * k, 2 * k + 1) for x in range(x_size)
        ]
        out_ref[:, k * 256 : (k + 1) * 256] = lax.dot_general(
            heads_out,
            jnp.concatenate(parts, axis=0),
            (((1,), (1,)), ((), ())),
            preferred_element_type=f32,
        ).astype(bf16)


def on_device(
    tokens,
    pre_gain,
    w_query,
    w_key,
    w_value,
    w_igate,
    w_fgate,
    forget_bias,
    gate_drift,
    head_gain,
    w_out,
):
    rows, width = tokens.shape
    z_size, x_size = lax.axis_size("z"), lax.axis_size("x")
    peers = z_size * x_size
    core = lax.axis_index("c")
    head = (lax.axis_index("y") * 2 + core).astype(jnp.int32).reshape(1)
    place = (lax.axis_index("z") * x_size + lax.axis_index("x")).astype(jnp.int32).reshape(1)
    smem = pl.BlockSpec(memory_space=pltpu.SMEM)
    vmem = pl.BlockSpec(memory_space=pltpu.VMEM)
    limit = pltpu.CompilerParams(vmem_limit_bytes=24 * 2**20)

    own_rows = pl.pallas_call(
        prepare_kernel,
        out_shape=pltpu.VMEM((8, rows, width + 128), bf16),
        in_specs=[smem] + [vmem] * 5,
        out_specs=vmem,
        compiler_params=limit,
        name="prepare",
    )(forget_bias, tokens, pre_gain.reshape(-1, 128), w_igate.T, w_fgate.T, gate_drift.T)
    with jax.named_scope("rows"):
        all_rows = lax.all_to_all(own_rows, ("c", "y"), split_axis=0, concat_axis=0, tiled=True)
    all_rows = near(all_rows.reshape(-1, width + 128))
    length = all_rows.shape[0]

    pair = jnp.stack(
        [
            jnp.concatenate(
                [
                    w_query[:, c * DK : (c + 1) * DK],
                    w_key[:, c * DK : (c + 1) * DK],
                    w_value[:, c * DV : (c + 1) * DV],
                    w_out[:, c * DV : (c + 1) * DV],
                ],
                axis=1,
            )
            for c in range(2)
        ]
    )
    with jax.named_scope("pair"):
        both = lax.all_gather(pair, "c", axis=0, tiled=False)
    mine = lax.dynamic_index_in_dim(both, core, axis=1, keepdims=False)
    mine = mine.reshape(-1, mine.shape[2])
    with jax.named_scope("along_z"):
        along_z = lax.all_gather(mine, "z", axis=0, tiled=True)
    cut = 2 * DK + DV

    def along_x(part):
        return lax.all_to_all(
            jnp.broadcast_to(part[None], (x_size,) + part.shape),
            "x",
            split_axis=0,
            concat_axis=0,
            tiled=True,
        )

    with jax.named_scope("w_in"):
        w_in = along_x(along_z[:, :cut])
    own_back = along_z[:, cut:]
    w_back = [own_back]
    for d in range(1, x_size):
        with jax.named_scope(f"w_back_{d}"):
            ring = [(k, (k + d) % x_size) for k in range(x_size)]
            w_back.append(lax.ppermute(own_back, "x", ring))

    pair_decay, aux, facts = pl.pallas_call(
        gates_kernel,
        out_shape=(
            pltpu.VMEM((length, length), f32),
            pltpu.VMEM((length, 128), f32),
            pltpu.VMEM((8, 128), f32),
        ),
        in_specs=[smem, vmem],
        out_specs=(vmem,) * 3,
        compiler_params=limit,
        name="gates",
    )(head, all_rows)
    query, key, value, message = pl.pallas_call(
        state_kernel,
        out_shape=(
            pltpu.VMEM((length, DK), bf16),
            pltpu.VMEM((length, DK), bf16),
            pltpu.VMEM((length, DV), bf16),
            pltpu.VMEM((peers * 8, DK), bf16),
        ),
        in_specs=[vmem] * 4,
        out_specs=(vmem,) * 4,
        scratch_shapes=[pltpu.VMEM((peers * 8, DK), f32)],
        compiler_params=limit,
        name="state",
    )(all_rows, near(w_in), aux, facts)
    with jax.named_scope("states_out"):
        arrived = lax.all_to_all(message, ROWS, split_axis=0, concat_axis=0, tiled=True)
    numer, denom = pl.pallas_call(
        intra_kernel,
        out_shape=(pltpu.VMEM((length, DV), f32), pltpu.VMEM((length, 128), f32)),
        in_specs=[vmem] * 4,
        out_specs=(vmem,) * 2,
        compiler_params=limit,
        name="intra",
    )(query, key, value, pair_decay)
    slices, entry = pl.pallas_call(
        prefix_kernel,
        out_shape=(pltpu.VMEM((DV, DK), f32), pltpu.VMEM((8, 128), f32)),
        in_specs=[smem, vmem],
        out_specs=(vmem,) * 2,
        scratch_shapes=[pltpu.VMEM((peers * 8, DK), f32)],
        compiler_params=limit,
        name="prefix",
    )(place, near(arrived))
    with jax.named_scope("states_back"):
        state = lax.all_to_all(slices, ROWS, split_axis=0, concat_axis=0, tiled=True)
    where = jnp.concatenate([head, lax.axis_index("x").astype(jnp.int32).reshape(1)])
    partial = pl.pallas_call(
        finish_kernel,
        out_shape=pltpu.VMEM((length, width), bf16),
        in_specs=[smem] + [vmem] * 11,
        out_specs=vmem,
        scratch_shapes=[pltpu.VMEM((x_size,) + own_back.shape, bf16)],
        compiler_params=limit,
        name="finish",
    )(
        where,
        query,
        numer,
        denom,
        aux,
        near(state),
        entry,
        head_gain.reshape(-1, 128),
        *[near(w) for w in w_back],
    )
    with jax.named_scope("heads"):
        halves = lax.all_to_all(
            partial.reshape(2, -1, width), "c", split_axis=0, concat_axis=0, tiled=True
        )
    joined = halves.astype(f32).sum(axis=0).astype(bf16)
    with jax.named_scope("owners"):
        pieces = lax.all_to_all(
            joined.reshape(-1, rows, width), "y", split_axis=0, concat_axis=0, tiled=True
        )
    return pieces.astype(f32).sum(axis=0).astype(bf16)


def solution(mesh):
    split = Mesh(mesh.devices.reshape(16, 4, 2, mesh.shape["tp"]), ("z", "x", "c", "y"))
    return jax.shard_map(
        on_device,
        mesh=split,
        in_specs=(
            P(SP_TP, None),
            P(),
            P(SP, "y"),
            P(SP, "y"),
            P(SP, "y"),
            P(),
            P(),
            P(),
            P(SP, None),
            P(),
            P(SP, "y"),
        ),
        out_specs=P(SP_TP, None),
        check_vma=False,
    )
```

```python
import jax
import jax.numpy as jnp
from jax import lax
from jax.experimental import pallas as pl
from jax.experimental.pallas import tpu as pltpu
from jax.sharding import Mesh
from jax.sharding import PartitionSpec as P

SP = ("z", "x", "c")
SP_TP = ("z", "x", "c", "y")
ROWS = ("z", "x")
HEADS = 8
DK = 128
DV = 256
norm_floor = 0.1
lowest_log = -1e30
highest = lax.Precision.HIGHEST
f32 = jnp.float32
bf16 = jnp.bfloat16


def near(array):
    return pltpu.with_memory_space_constraint(array, pltpu.VMEM)


def lane_ids(shape):
    return lax.broadcasted_iota(jnp.int32, shape, 1)


def row_ids(shape):
    return lax.broadcasted_iota(jnp.int32, shape, 0)


def three_parts(value):
    high = value.astype(bf16).astype(f32)
    middle = (value - high).astype(bf16).astype(f32)
    return high, middle, value - high - middle


def prepare_kernel(bias_ref, tokens_ref, gain_ref, w_igate_ref, w_fgate_ref, drift_ref, out_ref):
    wide = tokens_ref[...].astype(f32)
    scale = lax.rsqrt(jnp.mean(wide * wide, axis=1, keepdims=True) + norm_floor)
    gain = gain_ref[...].astype(f32)
    blocks = gain.shape[0]
    normed = jnp.concatenate(
        [
            (wide[:, k * 128 : (k + 1) * 128] * scale * gain[k : k + 1, :]).astype(bf16)
            for k in range(blocks)
        ],
        axis=1,
    )
    width = normed.shape[1]
    across = (((1,), (1,)), ((), ()))
    gate_in = lax.dot_general(w_igate_ref[...], normed, across, preferred_element_type=f32)
    forget = lax.dot_general(w_fgate_ref[...], normed, across, preferred_element_type=f32)
    heads = forget.shape[0]
    line = row_ids((heads, 1))
    bias = jnp.zeros((heads, 1), f32)
    for h in range(heads):
        bias = jnp.where(line == h, bias_ref[h], bias)
    forget = forget + bias + drift_ref[:, 0:1]
    log_forget = jnp.minimum(forget, 0.0) - jnp.log1p(jnp.exp(-jnp.abs(forget)))
    lane = lane_ids((heads, 128))
    row = row_ids((heads, 128))
    place_in = jnp.where(lane % 16 == row, 1.0, 0.0).astype(f32)
    place_forget = jnp.where(lane % 16 == row + heads, 1.0, 0.0).astype(f32)
    value = jnp.dot(
        gate_in.T, place_in, precision=highest, preferred_element_type=f32
    ) + jnp.dot(log_forget.T, place_forget, precision=highest, preferred_element_type=f32)
    high, middle, low = three_parts(value)
    lane = lane_ids(value.shape)
    piece = jnp.where(lane < 16, high, jnp.where(lane < 32, middle, low))
    piece = jnp.where(lane < 48, piece, 0.0).astype(bf16)
    for k in range(out_ref.shape[0]):
        out_ref[k, :, :width] = normed
        out_ref[k, :, width:] = piece


def gates_kernel(
    head_ref, rows_ref, along_ref, pair_ref, aux_ref, facts_ref, copies_ref, own_back_ref
):
    cut = copies_ref.shape[2]
    for k in range(copies_ref.shape[0]):
        copies_ref[k] = along_ref[:, :cut]
    own_back_ref[...] = along_ref[:, cut:]
    head = head_ref[0]
    gates = rows_ref[:, -128:].astype(f32)
    length = gates.shape[0]
    lane = lane_ids(gates.shape)
    input_col = jnp.sum(jnp.where(lane % 16 == head, gates, 0.0), axis=1, keepdims=True)
    forget_col = jnp.sum(jnp.where(lane % 16 == head + 8, gates, 0.0), axis=1, keepdims=True)
    both = jnp.where(lane == 0, input_col, jnp.where(lane == 1, forget_col, 0.0))
    both_rows = both.T
    input_row = both_rows[0:1, :]
    forget_row = both_rows[1:2, :]
    square = (length, length)
    s_id = row_ids(square)
    r_id = lane_ids(square)
    causal = r_id <= s_id
    up_to = jnp.where(causal, forget_row, 0.0)
    after = jnp.where(s_id > r_id, 1.0, 0.0).astype(f32)
    decay = jnp.dot(up_to, after, precision=highest, preferred_element_type=f32)
    within = jnp.sum(up_to, axis=1, keepdims=True)
    suffix = jnp.sum(jnp.where(r_id > s_id, forget_row, 0.0), axis=1, keepdims=True)
    log_pair = jnp.where(causal, decay + input_row, lowest_log)
    peak = jnp.max(log_pair, axis=1, keepdims=True)
    pair_ref[...] = jnp.where(causal, jnp.exp(log_pair - peak), 0.0)
    log_write = suffix + input_col
    top = jnp.max(log_write, axis=0, keepdims=True)
    write = jnp.exp(log_write - top)
    aux_ref[...] = jnp.where(
        lane == 1, peak, jnp.where(lane == 2, within, jnp.where(lane == 3, write, 0.0))
    )
    span_log = jnp.sum(forget_row, axis=1, keepdims=True)
    small = lane_ids(facts_ref.shape)
    facts = jnp.zeros(facts_ref.shape, f32)
    for k, piece in enumerate(three_parts(span_log) + three_parts(top)):
        facts = jnp.where(small == k, piece, facts)
    facts_ref[...] = facts


def column_of(aux, k):
    return jnp.sum(jnp.where(lane_ids(aux.shape) == k, aux, 0.0), axis=1, keepdims=True)


def state_kernel(
    rows_ref,
    w_ref,
    aux_ref,
    facts_ref,
    pair_ref,
    own_back_ref,
    query_ref,
    numer_ref,
    denom_ref,
    message_ref,
    passed_ref,
    buffer_ref,
):
    passed_ref[...] = own_back_ref[...]
    length, width = rows_ref.shape[0], rows_ref.shape[1] - 128
    x_size = w_ref.shape[0]
    run = 32
    total = jnp.zeros((length, w_ref.shape[2]), f32)
    for k in range(width // 256):
        parts = [
            w_ref[x, z * run : (z + 1) * run, :] for z in (2 * k, 2 * k + 1) for x in range(x_size)
        ]
        total = total + jnp.dot(
            rows_ref[:, k * 256 : (k + 1) * 256],
            jnp.concatenate(parts, axis=0),
            preferred_element_type=f32,
        )
    query = total[:, :DK].astype(bf16)
    query_ref[...] = query
    key = (total[:, DK : 2 * DK] * (DK**-0.5)).astype(bf16)
    value = total[:, 2 * DK :].astype(bf16)
    scaled_key = key.astype(f32) * column_of(aux_ref[...], 3)
    state = jnp.dot(value.astype(f32).T, scaled_key, precision=highest, preferred_element_type=f32)
    vector = jnp.sum(scaled_key, axis=0, keepdims=True)
    peers = buffer_ref.shape[0] // 8
    for r in range(DV // peers):
        buffer_ref[pl.ds(r, peers, stride=8), :] = state[r * peers : (r + 1) * peers, :]
    buffer_ref[pl.ds(4, peers, stride=8), :] = jnp.broadcast_to(vector, (peers, DK))
    buffer_ref[pl.ds(5, peers, stride=8), :] = jnp.broadcast_to(facts_ref[0:1, :], (peers, DK))
    for r in (6, 7):
        buffer_ref[pl.ds(r, peers, stride=8), :] = jnp.zeros((peers, DK), f32)
    message_ref[...] = buffer_ref[...].astype(bf16)
    scores = lax.dot_general(query, key, (((1,), (1,)), ((), ())), preferred_element_type=f32)
    weights = scores * pair_ref[...]
    numer_ref[...] = jnp.dot(weights.astype(bf16), value, preferred_element_type=f32)
    denom = jnp.sum(weights, axis=1, keepdims=True)
    denom_ref[...] = jnp.broadcast_to(denom, denom_ref.shape)


def prefix_kernel(
    place_ref, arrived_ref, own_back_ref, over_two_ref, out_ref, entry_ref, double_ref, buffer_ref
):
    double_ref[0] = own_back_ref[...]
    double_ref[1] = over_two_ref[...]
    place = place_ref[0]
    buffer_ref[...] = arrived_ref[...].astype(f32)
    peers = buffer_ref.shape[0] // 8
    vectors = buffer_ref[pl.ds(4, peers, stride=8), :]
    fact_rows = buffer_ref[pl.ds(5, peers, stride=8), :].T
    log_row = fact_rows[0:1, :] + fact_rows[1:2, :] + fact_rows[2:3, :]
    top_row = fact_rows[3:4, :] + fact_rows[4:5, :] + fact_rows[5:6, :]
    square = (peers, peers)
    i_id = row_ids(square)
    j_id = lane_ids(square)
    earlier = j_id < i_id
    before = jnp.where(earlier, log_row, 0.0)
    after = jnp.where(i_id > j_id, 1.0, 0.0).astype(f32)
    logs = jnp.dot(before, after, precision=highest, preferred_element_type=f32) + top_row
    logs = jnp.where(earlier, logs, lowest_log)
    top = jnp.max(logs, axis=1, keepdims=True)
    mix = jnp.where(earlier, jnp.exp(logs - top), 0.0)
    count = out_ref.shape[0] // peers
    for r in range(count):
        out_ref[pl.ds(r, peers, stride=count), :] = jnp.dot(
            mix,
            buffer_ref[pl.ds(r, peers, stride=8), :],
            precision=highest,
            preferred_element_type=f32,
        )
    entries = jnp.dot(mix, vectors, precision=highest, preferred_element_type=f32)
    mine = row_ids(entries.shape) == place
    vector = jnp.sum(jnp.where(mine, entries, 0.0), axis=0, keepdims=True)
    entry_top = jnp.sum(jnp.where(mine, top, 0.0), axis=0, keepdims=True)
    row = row_ids(entry_ref.shape)
    entry_ref[...] = jnp.where(row == 0, vector, jnp.where(row == 1, entry_top, 0.0))


def finish_kernel(
    head_ref,
    query_ref,
    numer_ref,
    denom_ref,
    aux_ref,
    state_ref,
    entry_ref,
    gain_ref,
    double_ref,
    next_ref,
    out_ref,
    w_ref,
):
    head = head_ref[0]
    my_x = head_ref[1]
    for k in range(2):
        w_ref[(my_x + 2 * k) % 4] = double_ref[k]
        w_ref[(my_x + 3 + 2 * k) % 4] = next_ref[k]
    peers = 64
    count = state_ref.shape[0] // peers
    state = jnp.concatenate(
        [state_ref[pl.ds(r, peers, stride=count), :] for r in range(count)], axis=0
    )
    query = query_ref[...].astype(f32)
    left = lax.dot_general(
        query, state, (((1,), (1,)), ((), ())), precision=highest, preferred_element_type=f32
    )
    entry_vec = entry_ref[0:1, :]
    entry_top = entry_ref[1:2, 0:1]
    left_denom = jnp.sum(query * entry_vec, axis=1, keepdims=True)
    aux = aux_ref[...]
    denom = denom_ref[:, 0:1]
    peak = column_of(aux, 1)
    carried = column_of(aux, 2) + entry_top
    top = jnp.maximum(peak, carried)
    own = jnp.exp(peak - top)
    old = jnp.exp(carried - top)
    numer = own * numer_ref[...] + old * left
    denom = own * denom + old * left_denom
    hidden = numer / jnp.maximum(jnp.abs(denom), jnp.exp(-top))
    gains = gain_ref[...].astype(f32)
    row = row_ids(gains.shape)
    gain = jnp.concatenate(
        [
            jnp.sum(jnp.where(row == 2 * head + k, gains, 0.0), axis=0, keepdims=True)
            for k in range(2)
        ],
        axis=1,
    )
    scale = lax.rsqrt(jnp.mean(hidden * hidden, axis=1, keepdims=True) + norm_floor)
    heads_out = (hidden * scale * gain).astype(bf16)
    x_size = w_ref.shape[0]
    run = 32
    for k in range(out_ref.shape[1] // 256):
        parts = [
            w_ref[x, z * run : (z + 1) * run, :] for z in (2 * k, 2 * k + 1) for x in range(x_size)
        ]
        out_ref[:, k * 256 : (k + 1) * 256] = lax.dot_general(
            heads_out,
            jnp.concatenate(parts, axis=0),
            (((1,), (1,)), ((), ())),
            preferred_element_type=f32,
        ).astype(bf16)


def on_device(
    tokens,
    pre_gain,
    w_query,
    w_key,
    w_value,
    w_igate,
    w_fgate,
    forget_bias,
    gate_drift,
    head_gain,
    w_out,
):
    rows, width = tokens.shape
    z_size, x_size = lax.axis_size("z"), lax.axis_size("x")
    peers = z_size * x_size
    core = lax.axis_index("c")
    head = (lax.axis_index("y") * 2 + core).astype(jnp.int32).reshape(1)
    place = (lax.axis_index("z") * x_size + lax.axis_index("x")).astype(jnp.int32).reshape(1)
    smem = pl.BlockSpec(memory_space=pltpu.SMEM)
    vmem = pl.BlockSpec(memory_space=pltpu.VMEM)
    limit = pltpu.CompilerParams(vmem_limit_bytes=24 * 2**20)

    own_rows = pl.pallas_call(
        prepare_kernel,
        out_shape=pltpu.VMEM((8, rows, width + 128), bf16),
        in_specs=[smem] + [vmem] * 5,
        out_specs=vmem,
        name="prepare",
    )(forget_bias, tokens, pre_gain.reshape(-1, 128), w_igate.T, w_fgate.T, gate_drift.T)
    with jax.named_scope("rows"):
        all_rows = lax.all_to_all(own_rows, ("c", "y"), split_axis=0, concat_axis=0, tiled=True)
    all_rows = near(all_rows.reshape(-1, width + 128))
    length = all_rows.shape[0]

    pair = jnp.stack(
        [
            jnp.concatenate(
                [
                    w_query[:, c * DK : (c + 1) * DK],
                    w_key[:, c * DK : (c + 1) * DK],
                    w_value[:, c * DV : (c + 1) * DV],
                    w_out[:, c * DV : (c + 1) * DV],
                ],
                axis=1,
            )
            for c in range(2)
        ]
    )
    with jax.named_scope("pair"):
        both = lax.all_gather(pair, "c", axis=0, tiled=False)
    mine = lax.dynamic_index_in_dim(both, core, axis=1, keepdims=False)
    mine = mine.reshape(-1, mine.shape[2])
    with jax.named_scope("along_z"):
        along_z = lax.all_gather(mine, "z", axis=0, tiled=True)
    cut = 2 * DK + DV

    pair_decay, aux, facts, copies, own_back = pl.pallas_call(
        gates_kernel,
        out_shape=(
            pltpu.VMEM((length, length), f32),
            pltpu.VMEM((length, 128), f32),
            pltpu.VMEM((8, 128), f32),
            pltpu.VMEM((x_size, along_z.shape[0], cut), bf16),
            pltpu.VMEM((along_z.shape[0], along_z.shape[1] - cut), bf16),
        ),
        in_specs=[smem, vmem, vmem],
        out_specs=(vmem,) * 5,
        compiler_params=limit,
        name="gates",
    )(head, all_rows, near(along_z))
    with jax.named_scope("w_in"):
        w_in = lax.all_to_all(copies, "x", split_axis=0, concat_axis=0, tiled=True)
    query, numer, denom, message, own_back = pl.pallas_call(
        state_kernel,
        out_shape=(
            pltpu.VMEM((length, DK), bf16),
            pltpu.VMEM((length, DV), f32),
            pltpu.VMEM((length, 128), f32),
            pltpu.VMEM((peers * 8, DK), bf16),
            pltpu.VMEM(own_back.shape, bf16),
        ),
        in_specs=[vmem] * 6,
        out_specs=(vmem,) * 5,
        scratch_shapes=[pltpu.VMEM((peers * 8, DK), f32)],
        compiler_params=limit,
        name="state",
    )(all_rows, near(w_in), aux, facts, pair_decay, own_back)
    with jax.named_scope("states_out"):
        arrived = lax.all_to_all(message, ROWS, split_axis=0, concat_axis=0, tiled=True)

    def ring(d):
        return [(k, (k + d) % x_size) for k in range(x_size)]

    with jax.named_scope("over_two"):
        over_two = lax.ppermute(own_back, "x", ring(2))
    slices, entry, double = pl.pallas_call(
        prefix_kernel,
        out_shape=(
            pltpu.VMEM((DV, DK), f32),
            pltpu.VMEM((8, 128), f32),
            pltpu.VMEM((2,) + own_back.shape, bf16),
        ),
        in_specs=[smem, vmem, vmem, vmem],
        out_specs=(vmem,) * 3,
        scratch_shapes=[pltpu.VMEM((peers * 8, DK), f32)],
        compiler_params=limit,
        name="prefix",
    )(place, near(arrived), own_back, near(over_two))
    with jax.named_scope("states_back"):
        state = lax.all_to_all(slices, ROWS, split_axis=0, concat_axis=0, tiled=True)
    with jax.named_scope("over_one"):
        following = lax.ppermute(double, "x", ring(1))
    where = jnp.concatenate([head, lax.axis_index("x").astype(jnp.int32).reshape(1)])
    partial = pl.pallas_call(
        finish_kernel,
        out_shape=pltpu.VMEM((length, width), bf16),
        in_specs=[smem] + [vmem] * 9,
        out_specs=vmem,
        scratch_shapes=[pltpu.VMEM((x_size,) + own_back.shape, bf16)],
        compiler_params=limit,
        name="finish",
    )(
        where,
        query,
        numer,
        denom,
        aux,
        near(state),
        entry,
        head_gain.reshape(-1, 128),
        double,
        near(following),
    )
    with jax.named_scope("heads"):
        halves = lax.all_to_all(
            partial.reshape(2, -1, width), "c", split_axis=0, concat_axis=0, tiled=True
        )
    joined = halves.astype(f32).sum(axis=0).astype(bf16)
    with jax.named_scope("owners"):
        pieces = lax.all_to_all(
            joined.reshape(-1, rows, width), "y", split_axis=0, concat_axis=0, tiled=True
        )
    return pieces.astype(f32).sum(axis=0).astype(bf16)


def solution(mesh):
    split = Mesh(mesh.devices.reshape(16, 4, 2, mesh.shape["tp"]), ("z", "x", "c", "y"))
    return jax.shard_map(
        on_device,
        mesh=split,
        in_specs=(
            P(SP_TP, None),
            P(),
            P(SP, "y"),
            P(SP, "y"),
            P(SP, "y"),
            P(),
            P(),
            P(),
            P(SP, None),
            P(),
            P(SP, "y"),
        ),
        out_specs=P(SP_TP, None),
        check_vma=False,
    )
```

```python
import jax
import jax.numpy as jnp
from jax import lax
from jax.experimental import pallas as pl
from jax.experimental.pallas import tpu as pltpu
from jax.sharding import Mesh
from jax.sharding import PartitionSpec as P

SP = ("z", "x", "c")
SP_TP = ("z", "x", "c", "y")
ROWS = ("z", "x")
DK = 128
DV = 256
norm_floor = 0.1
lowest_log = -1e30
highest = lax.Precision.HIGHEST
f32 = jnp.float32
bf16 = jnp.bfloat16


def near(array):
    return pltpu.with_memory_space_constraint(array, pltpu.VMEM)


def lane_ids(shape):
    return lax.broadcasted_iota(jnp.int32, shape, 1)


def row_ids(shape):
    return lax.broadcasted_iota(jnp.int32, shape, 0)


def three_parts(value):
    high = value.astype(bf16).astype(f32)
    middle = (value - high).astype(bf16).astype(f32)
    return high, middle, value - high - middle


def prepare_kernel(bias_ref, tokens_ref, gain_ref, w_igate_ref, w_fgate_ref, drift_ref, out_ref):
    wide = tokens_ref[...].astype(f32)
    scale = lax.rsqrt(jnp.mean(wide * wide, axis=1, keepdims=True) + norm_floor)
    gain = gain_ref[...].astype(f32)
    blocks = gain.shape[0]
    normed = jnp.concatenate(
        [
            (wide[:, k * 128 : (k + 1) * 128] * scale * gain[k : k + 1, :]).astype(bf16)
            for k in range(blocks)
        ],
        axis=1,
    )
    width = normed.shape[1]
    across = (((1,), (1,)), ((), ()))
    gate_in = lax.dot_general(w_igate_ref[...], normed, across, preferred_element_type=f32)
    forget = lax.dot_general(w_fgate_ref[...], normed, across, preferred_element_type=f32)
    heads = forget.shape[0]
    line = row_ids((heads, 1))
    bias = jnp.zeros((heads, 1), f32)
    for h in range(heads):
        bias = jnp.where(line == h, bias_ref[h], bias)
    forget = forget + bias + drift_ref[:, 0:1]
    log_forget = jnp.minimum(forget, 0.0) - jnp.log1p(jnp.exp(-jnp.abs(forget)))
    lane = lane_ids((heads, 128))
    row = row_ids((heads, 128))
    place_in = jnp.where(lane % 16 == row, 1.0, 0.0).astype(f32)
    place_forget = jnp.where(lane % 16 == row + heads, 1.0, 0.0).astype(f32)
    value = jnp.dot(
        gate_in.T, place_in, precision=highest, preferred_element_type=f32
    ) + jnp.dot(log_forget.T, place_forget, precision=highest, preferred_element_type=f32)
    high, middle, low = three_parts(value)
    lane = lane_ids(value.shape)
    piece = jnp.where(lane < 16, high, jnp.where(lane < 32, middle, low))
    piece = jnp.where(lane < 48, piece, 0.0).astype(bf16)
    for k in range(out_ref.shape[0]):
        out_ref[k, :, :width] = normed
        out_ref[k, :, width:] = piece


def gates_kernel(
    head_ref, rows_ref, along_ref, pair_ref, aux_ref, facts_ref, copies_ref, own_ref
):
    cut = copies_ref.shape[2]
    for k in range(copies_ref.shape[0]):
        copies_ref[k] = along_ref[:, :cut]
    own_ref[...] = along_ref[:, cut:]
    head = head_ref[0]
    gates = rows_ref[:, -128:].astype(f32)
    length = gates.shape[0]
    lane = lane_ids(gates.shape)
    input_col = jnp.sum(jnp.where(lane % 16 == head, gates, 0.0), axis=1, keepdims=True)
    forget_col = jnp.sum(jnp.where(lane % 16 == head + 8, gates, 0.0), axis=1, keepdims=True)
    both = jnp.where(lane == 0, input_col, jnp.where(lane == 1, forget_col, 0.0))
    both_rows = both.T
    input_row = both_rows[0:1, :]
    forget_row = both_rows[1:2, :]
    square = (length, length)
    s_id = row_ids(square)
    r_id = lane_ids(square)
    causal = r_id <= s_id
    up_to = jnp.where(causal, forget_row, 0.0)
    after = jnp.where(s_id > r_id, 1.0, 0.0).astype(f32)
    decay = jnp.dot(up_to, after, precision=highest, preferred_element_type=f32)
    within = jnp.sum(up_to, axis=1, keepdims=True)
    suffix = jnp.sum(jnp.where(r_id > s_id, forget_row, 0.0), axis=1, keepdims=True)
    log_pair = jnp.where(causal, decay + input_row, lowest_log)
    peak = jnp.max(log_pair, axis=1, keepdims=True)
    pair_ref[...] = jnp.where(causal, jnp.exp(log_pair - peak), 0.0)
    log_write = suffix + input_col
    top = jnp.max(log_write, axis=0, keepdims=True)
    write = jnp.exp(log_write - top)
    aux_ref[...] = jnp.where(
        lane == 1, peak, jnp.where(lane == 2, within, jnp.where(lane == 3, write, 0.0))
    )
    span_log = jnp.sum(forget_row, axis=1, keepdims=True)
    small = lane_ids(facts_ref.shape)
    facts = jnp.zeros(facts_ref.shape, f32)
    for k, piece in enumerate(three_parts(span_log) + three_parts(top)):
        facts = jnp.where(small == k, piece, facts)
    facts_ref[...] = facts


def column_of(aux, k):
    return jnp.sum(jnp.where(lane_ids(aux.shape) == k, aux, 0.0), axis=1, keepdims=True)


def projected(rows_ref, w_ref, start, stop, width):
    x_size = w_ref.shape[0]
    run = 32
    total = jnp.zeros((rows_ref.shape[0], stop - start), f32)
    for k in range(width // 256):
        parts = [
            w_ref[x, z * run : (z + 1) * run, start:stop]
            for z in (2 * k, 2 * k + 1)
            for x in range(x_size)
        ]
        total = total + jnp.dot(
            rows_ref[:, k * 256 : (k + 1) * 256],
            jnp.concatenate(parts, axis=0),
            preferred_element_type=f32,
        )
    return total


def state_kernel(
    rows_ref,
    w_ref,
    aux_ref,
    facts_ref,
    own_ref,
    key_ref,
    value_ref,
    message_ref,
    passed_ref,
    buffer_ref,
):
    passed_ref[...] = own_ref[...]
    width = rows_ref.shape[1] - 128
    total = projected(rows_ref, w_ref, 0, DK + DV, width)
    key = (total[:, :DK] * (DK**-0.5)).astype(bf16)
    value = total[:, DK:].astype(bf16)
    key_ref[...] = key
    value_ref[...] = value
    scaled_key = key.astype(f32) * column_of(aux_ref[...], 3)
    state = jnp.dot(value.astype(f32).T, scaled_key, precision=highest, preferred_element_type=f32)
    vector = jnp.sum(scaled_key, axis=0, keepdims=True)
    peers = buffer_ref.shape[0] // 8
    for r in range(DV // peers):
        buffer_ref[pl.ds(r, peers, stride=8), :] = state[r * peers : (r + 1) * peers, :]
    buffer_ref[pl.ds(4, peers, stride=8), :] = jnp.broadcast_to(vector, (peers, DK))
    buffer_ref[pl.ds(5, peers, stride=8), :] = jnp.broadcast_to(facts_ref[0:1, :], (peers, DK))
    for r in (6, 7):
        buffer_ref[pl.ds(r, peers, stride=8), :] = jnp.zeros((peers, DK), f32)
    message_ref[...] = buffer_ref[...].astype(bf16)


def prefix_kernel(
    place_ref,
    arrived_ref,
    before_ref,
    behind_ref,
    out_ref,
    entry_ref,
    upper_ref,
    lower_ref,
    buffer_ref,
):
    half = upper_ref.shape[0]
    upper_ref[...] = before_ref[:half, :]
    lower_ref[...] = behind_ref[half:, :]
    place = place_ref[0]
    buffer_ref[...] = arrived_ref[...].astype(f32)
    peers = buffer_ref.shape[0] // 8
    vectors = buffer_ref[pl.ds(4, peers, stride=8), :]
    fact_rows = buffer_ref[pl.ds(5, peers, stride=8), :].T
    log_row = fact_rows[0:1, :] + fact_rows[1:2, :] + fact_rows[2:3, :]
    top_row = fact_rows[3:4, :] + fact_rows[4:5, :] + fact_rows[5:6, :]
    square = (peers, peers)
    i_id = row_ids(square)
    j_id = lane_ids(square)
    earlier = j_id < i_id
    before = jnp.where(earlier, log_row, 0.0)
    after = jnp.where(i_id > j_id, 1.0, 0.0).astype(f32)
    logs = jnp.dot(before, after, precision=highest, preferred_element_type=f32) + top_row
    logs = jnp.where(earlier, logs, lowest_log)
    top = jnp.max(logs, axis=1, keepdims=True)
    mix = jnp.where(earlier, jnp.exp(logs - top), 0.0)
    count = out_ref.shape[0] // peers
    for r in range(count):
        out_ref[pl.ds(r, peers, stride=count), :] = jnp.dot(
            mix,
            buffer_ref[pl.ds(r, peers, stride=8), :],
            precision=highest,
            preferred_element_type=f32,
        )
    entries = jnp.dot(mix, vectors, precision=highest, preferred_element_type=f32)
    mine = row_ids(entries.shape) == place
    vector = jnp.sum(jnp.where(mine, entries, 0.0), axis=0, keepdims=True)
    entry_top = jnp.sum(jnp.where(mine, top, 0.0), axis=0, keepdims=True)
    row = row_ids(entry_ref.shape)
    entry_ref[...] = jnp.where(row == 0, vector, jnp.where(row == 1, entry_top, 0.0))


def finish_kernel(
    head_ref,
    rows_ref,
    key_ref,
    value_ref,
    pair_ref,
    aux_ref,
    state_ref,
    entry_ref,
    gain_ref,
    own_ref,
    before_ref,
    behind_ref,
    upper_ref,
    lower_ref,
    out_ref,
    w_ref,
):
    head = head_ref[0]
    my_x = head_ref[1]
    half = upper_ref.shape[0]
    w_ref[my_x] = own_ref[...]
    w_ref[(my_x + 3) % 4] = before_ref[...]
    w_ref[(my_x + 1) % 4] = behind_ref[...]
    w_ref[(my_x + 2) % 4, :half, :] = upper_ref[...]
    w_ref[(my_x + 2) % 4, half:, :] = lower_ref[...]
    width = out_ref.shape[1]
    query_low = projected(rows_ref, w_ref, 0, DK, width).astype(bf16)
    scores = lax.dot_general(
        query_low, key_ref[...], (((1,), (1,)), ((), ())), preferred_element_type=f32
    )
    weights = scores * pair_ref[...]
    numer = jnp.dot(weights.astype(bf16), value_ref[...], preferred_element_type=f32)
    denom = jnp.sum(weights, axis=1, keepdims=True)
    peers = 64
    count = state_ref.shape[0] // peers
    state = jnp.concatenate(
        [state_ref[pl.ds(r, peers, stride=count), :] for r in range(count)], axis=0
    )
    query = query_low.astype(f32)
    left = lax.dot_general(
        query, state, (((1,), (1,)), ((), ())), precision=highest, preferred_element_type=f32
    )
    entry_vec = entry_ref[0:1, :]
    entry_top = entry_ref[1:2, 0:1]
    left_denom = jnp.sum(query * entry_vec, axis=1, keepdims=True)
    aux = aux_ref[...]
    peak = column_of(aux, 1)
    carried = column_of(aux, 2) + entry_top
    top = jnp.maximum(peak, carried)
    own = jnp.exp(peak - top)
    old = jnp.exp(carried - top)
    numer = own * numer + old * left
    denom = own * denom + old * left_denom
    hidden = numer / jnp.maximum(jnp.abs(denom), jnp.exp(-top))
    gains = gain_ref[...].astype(f32)
    row = row_ids(gains.shape)
    gain = jnp.concatenate(
        [
            jnp.sum(jnp.where(row == 2 * head + k, gains, 0.0), axis=0, keepdims=True)
            for k in range(2)
        ],
        axis=1,
    )
    scale = lax.rsqrt(jnp.mean(hidden * hidden, axis=1, keepdims=True) + norm_floor)
    heads_out = (hidden * scale * gain).astype(bf16)
    x_size = w_ref.shape[0]
    run = 32
    for k in range(out_ref.shape[1] // 256):
        parts = [
            w_ref[x, z * run : (z + 1) * run, DK:]
            for z in (2 * k, 2 * k + 1)
            for x in range(x_size)
        ]
        out_ref[:, k * 256 : (k + 1) * 256] = lax.dot_general(
            heads_out,
            jnp.concatenate(parts, axis=0),
            (((1,), (1,)), ((), ())),
            preferred_element_type=f32,
        ).astype(bf16)


def on_device(
    tokens,
    pre_gain,
    w_query,
    w_key,
    w_value,
    w_igate,
    w_fgate,
    forget_bias,
    gate_drift,
    head_gain,
    w_out,
):
    rows, width = tokens.shape
    z_size, x_size = lax.axis_size("z"), lax.axis_size("x")
    peers = z_size * x_size
    core = lax.axis_index("c")
    head = (lax.axis_index("y") * 2 + core).astype(jnp.int32).reshape(1)
    place = (lax.axis_index("z") * x_size + lax.axis_index("x")).astype(jnp.int32).reshape(1)
    smem = pl.BlockSpec(memory_space=pltpu.SMEM)
    vmem = pl.BlockSpec(memory_space=pltpu.VMEM)
    limit = pltpu.CompilerParams(vmem_limit_bytes=24 * 2**20)

    own_rows = pl.pallas_call(
        prepare_kernel,
        out_shape=pltpu.VMEM((8, rows, width + 128), bf16),
        in_specs=[smem] + [vmem] * 5,
        out_specs=vmem,
        name="prepare",
    )(forget_bias, tokens, pre_gain.reshape(-1, 128), w_igate.T, w_fgate.T, gate_drift.T)
    all_rows = lax.all_to_all(own_rows, ("c", "y"), split_axis=0, concat_axis=0, tiled=True)
    all_rows = near(all_rows.reshape(-1, width + 128))
    length = all_rows.shape[0]

    pair = jnp.stack(
        [
            jnp.concatenate(
                [
                    w_key[:, c * DK : (c + 1) * DK],
                    w_value[:, c * DV : (c + 1) * DV],
                    w_query[:, c * DK : (c + 1) * DK],
                    w_out[:, c * DV : (c + 1) * DV],
                ],
                axis=1,
            )
            for c in range(2)
        ]
    )
    both = lax.all_gather(pair, "c", axis=0, tiled=False)
    mine = lax.dynamic_index_in_dim(both, core, axis=1, keepdims=False)
    mine = mine.reshape(-1, mine.shape[2])
    along_z = lax.all_gather(mine, "z", axis=0, tiled=True)
    cut = DK + DV

    rest = (along_z.shape[0], along_z.shape[1] - cut)
    pair_decay, aux, facts, copies, own_rest = pl.pallas_call(
        gates_kernel,
        out_shape=(
            pltpu.VMEM((length, length), f32),
            pltpu.VMEM((length, 128), f32),
            pltpu.VMEM((8, 128), f32),
            pltpu.VMEM((x_size, along_z.shape[0], cut), bf16),
            pltpu.VMEM(rest, bf16),
        ),
        in_specs=[smem, vmem, vmem],
        out_specs=(vmem,) * 5,
        compiler_params=limit,
        name="gates",
    )(head, all_rows, near(along_z))
    w_in = lax.all_to_all(copies, "x", split_axis=0, concat_axis=0, tiled=True)
    key, value, message, own_rest = pl.pallas_call(
        state_kernel,
        out_shape=(
            pltpu.VMEM((length, DK), bf16),
            pltpu.VMEM((length, DV), bf16),
            pltpu.VMEM((peers * 8, DK), bf16),
            pltpu.VMEM(rest, bf16),
        ),
        in_specs=[vmem] * 5,
        out_specs=(vmem,) * 4,
        scratch_shapes=[pltpu.VMEM((peers * 8, DK), f32)],
        compiler_params=limit,
        name="state",
    )(all_rows, near(w_in), aux, facts, own_rest)
    arrived = lax.all_to_all(message, ROWS, split_axis=0, concat_axis=0, tiled=True)

    def ring(d):
        return [(k, (k + d) % x_size) for k in range(x_size)]

    before = near(lax.ppermute(own_rest, "x", ring(1)))
    behind = near(lax.ppermute(own_rest, "x", ring(-1)))
    half = (rest[0] // 2, rest[1])
    slices, entry, upper, lower = pl.pallas_call(
        prefix_kernel,
        out_shape=(
            pltpu.VMEM((DV, DK), f32),
            pltpu.VMEM((8, 128), f32),
            pltpu.VMEM(half, bf16),
            pltpu.VMEM(half, bf16),
        ),
        in_specs=[smem, vmem, vmem, vmem],
        out_specs=(vmem,) * 4,
        scratch_shapes=[pltpu.VMEM((peers * 8, DK), f32)],
        compiler_params=limit,
        name="prefix",
    )(place, near(arrived), before, behind)
    state = lax.all_to_all(slices, ROWS, split_axis=0, concat_axis=0, tiled=True)
    upper = near(lax.ppermute(upper, "x", ring(1)))
    lower = near(lax.ppermute(lower, "x", ring(-1)))
    where = jnp.concatenate([head, lax.axis_index("x").astype(jnp.int32).reshape(1)])
    partial = pl.pallas_call(
        finish_kernel,
        out_shape=pltpu.VMEM((length, width), bf16),
        in_specs=[smem] + [vmem] * 13,
        out_specs=vmem,
        scratch_shapes=[pltpu.VMEM((x_size,) + rest, bf16)],
        compiler_params=limit,
        name="finish",
    )(
        where,
        all_rows,
        key,
        value,
        pair_decay,
        aux,
        near(state),
        entry,
        head_gain.reshape(-1, 128),
        own_rest,
        before,
        behind,
        upper,
        lower,
    )
    halves = lax.all_to_all(
        partial.reshape(2, -1, width), "c", split_axis=0, concat_axis=0, tiled=True
    )
    joined = halves.astype(f32).sum(axis=0).astype(bf16)
    pieces = lax.all_to_all(
        joined.reshape(-1, rows, width), "y", split_axis=0, concat_axis=0, tiled=True
    )
    return pieces.astype(f32).sum(axis=0).astype(bf16)


def solution(mesh):
    split = Mesh(mesh.devices.reshape(16, 4, 2, mesh.shape["tp"]), ("z", "x", "c", "y"))
    return jax.shard_map(
        on_device,
        mesh=split,
        in_specs=(
            P(SP_TP, None),
            P(),
            P(SP, "y"),
            P(SP, "y"),
            P(SP, "y"),
            P(),
            P(),
            P(),
            P(SP, None),
            P(),
            P(SP, "y"),
        ),
        out_specs=P(SP_TP, None),
        check_vma=False,
    )
```

```python
import jax
import jax.numpy as jnp
from jax import lax
from jax.experimental import pallas as pl
from jax.experimental.pallas import tpu as pltpu
from jax.sharding import Mesh
from jax.sharding import PartitionSpec as P

SP = ("z", "x", "c")
SP_TP = ("z", "x", "c", "y")
ROWS = ("z", "x")
DK = 128
DV = 256
FIRST_ROWS = 320
norm_floor = 0.1
lowest_log = -1e30
highest = lax.Precision.HIGHEST
f32 = jnp.float32
bf16 = jnp.bfloat16


def near(array):
    return pltpu.with_memory_space_constraint(array, pltpu.VMEM)


def lane_ids(shape):
    return lax.broadcasted_iota(jnp.int32, shape, 1)


def row_ids(shape):
    return lax.broadcasted_iota(jnp.int32, shape, 0)


def three_parts(value):
    high = value.astype(bf16).astype(f32)
    middle = (value - high).astype(bf16).astype(f32)
    return high, middle, value - high - middle


def prepare_kernel(bias_ref, tokens_ref, gain_ref, w_igate_ref, w_fgate_ref, drift_ref, out_ref):
    wide = tokens_ref[...].astype(f32)
    scale = lax.rsqrt(jnp.mean(wide * wide, axis=1, keepdims=True) + norm_floor)
    gain = gain_ref[...].astype(f32)
    blocks = gain.shape[0]
    normed = jnp.concatenate(
        [
            (wide[:, k * 128 : (k + 1) * 128] * scale * gain[k : k + 1, :]).astype(bf16)
            for k in range(blocks)
        ],
        axis=1,
    )
    width = normed.shape[1]
    across = (((1,), (1,)), ((), ()))
    gate_in = lax.dot_general(w_igate_ref[...], normed, across, preferred_element_type=f32)
    forget = lax.dot_general(w_fgate_ref[...], normed, across, preferred_element_type=f32)
    heads = forget.shape[0]
    line = row_ids((heads, 1))
    bias = jnp.zeros((heads, 1), f32)
    for h in range(heads):
        bias = jnp.where(line == h, bias_ref[h], bias)
    forget = forget + bias + drift_ref[:, 0:1]
    log_forget = jnp.minimum(forget, 0.0) - jnp.log1p(jnp.exp(-jnp.abs(forget)))
    lane = lane_ids((heads, 128))
    row = row_ids((heads, 128))
    place_in = jnp.where(lane % 16 == row, 1.0, 0.0).astype(f32)
    place_forget = jnp.where(lane % 16 == row + heads, 1.0, 0.0).astype(f32)
    value = jnp.dot(
        gate_in.T, place_in, precision=highest, preferred_element_type=f32
    ) + jnp.dot(log_forget.T, place_forget, precision=highest, preferred_element_type=f32)
    high, middle, low = three_parts(value)
    lane = lane_ids(value.shape)
    piece = jnp.where(lane < 16, high, jnp.where(lane < 32, middle, low))
    piece = jnp.where(lane < 48, piece, 0.0).astype(bf16)
    for k in range(out_ref.shape[0]):
        out_ref[k, :, :width] = normed
        out_ref[k, :, width:] = piece


def gates_kernel(
    head_ref, rows_ref, along_ref, pair_ref, aux_ref, facts_ref, copies_ref, rest_ref
):
    cut = copies_ref.shape[2]
    for k in range(copies_ref.shape[0]):
        copies_ref[k] = along_ref[:, :cut]
    rest_ref[...] = along_ref[:, cut:]
    head = head_ref[0]
    gates = rows_ref[:, -128:].astype(f32)
    length = gates.shape[0]
    lane = lane_ids(gates.shape)
    input_col = jnp.sum(jnp.where(lane % 16 == head, gates, 0.0), axis=1, keepdims=True)
    forget_col = jnp.sum(jnp.where(lane % 16 == head + 8, gates, 0.0), axis=1, keepdims=True)
    both = jnp.where(lane == 0, input_col, jnp.where(lane == 1, forget_col, 0.0))
    both_rows = both.T
    input_row = both_rows[0:1, :]
    forget_row = both_rows[1:2, :]
    square = (length, length)
    s_id = row_ids(square)
    r_id = lane_ids(square)
    causal = r_id <= s_id
    up_to = jnp.where(causal, forget_row, 0.0)
    after = jnp.where(s_id > r_id, 1.0, 0.0).astype(f32)
    decay = jnp.dot(up_to, after, precision=highest, preferred_element_type=f32)
    within = jnp.sum(up_to, axis=1, keepdims=True)
    suffix = jnp.sum(jnp.where(r_id > s_id, forget_row, 0.0), axis=1, keepdims=True)
    log_pair = jnp.where(causal, decay + input_row, lowest_log)
    peak = jnp.max(log_pair, axis=1, keepdims=True)
    pair_ref[...] = jnp.where(causal, jnp.exp(log_pair - peak), 0.0)
    log_write = suffix + input_col
    top = jnp.max(log_write, axis=0, keepdims=True)
    write = jnp.exp(log_write - top)
    aux_ref[...] = jnp.where(
        lane == 1, peak, jnp.where(lane == 2, within, jnp.where(lane == 3, write, 0.0))
    )
    span_log = jnp.sum(forget_row, axis=1, keepdims=True)
    small = lane_ids(facts_ref.shape)
    facts = jnp.zeros(facts_ref.shape, f32)
    for k, piece in enumerate(three_parts(span_log) + three_parts(top)):
        facts = jnp.where(small == k, piece, facts)
    facts_ref[...] = facts


def column_of(aux, k):
    return jnp.sum(jnp.where(lane_ids(aux.shape) == k, aux, 0.0), axis=1, keepdims=True)


def weight_rows(pieces, k, start, stop):
    parts = []
    for z in (2 * k, 2 * k + 1):
        at, piece = 32 * z, pieces[0]
        if at >= piece.shape[1]:
            at, piece = at - piece.shape[1], pieces[1]
        for x in range(piece.shape[0]):
            parts.append(piece[x, at : at + 32, start:stop])
    return jnp.concatenate(parts, axis=0)


def projected(rows_ref, pieces, start, stop, width):
    total = jnp.zeros((rows_ref.shape[0], stop - start), f32)
    for k in range(width // 256):
        total = total + jnp.dot(
            rows_ref[:, k * 256 : (k + 1) * 256],
            weight_rows(pieces, k, start, stop),
            preferred_element_type=f32,
        )
    return total


def state_kernel(
    rows_ref,
    w_ref,
    aux_ref,
    facts_ref,
    rest_ref,
    key_ref,
    value_ref,
    message_ref,
    first_ref,
    second_ref,
    buffer_ref,
):
    cut = first_ref.shape[0]
    first_ref[...] = rest_ref[:cut, :]
    second_ref[...] = rest_ref[cut:, :]
    width = rows_ref.shape[1] - 128
    total = projected(rows_ref, (w_ref,), 0, DK + DV, width)
    key = (total[:, :DK] * (DK**-0.5)).astype(bf16)
    value = total[:, DK:].astype(bf16)
    key_ref[...] = key
    value_ref[...] = value
    scaled_key = key.astype(f32) * column_of(aux_ref[...], 3)
    state = jnp.dot(value.astype(f32).T, scaled_key, precision=highest, preferred_element_type=f32)
    vector = jnp.sum(scaled_key, axis=0, keepdims=True)
    peers = buffer_ref.shape[0] // 8
    for r in range(DV // peers):
        buffer_ref[pl.ds(r, peers, stride=8), :] = state[r * peers : (r + 1) * peers, :]
    buffer_ref[pl.ds(4, peers, stride=8), :] = jnp.broadcast_to(vector, (peers, DK))
    buffer_ref[pl.ds(5, peers, stride=8), :] = jnp.broadcast_to(facts_ref[0:1, :], (peers, DK))
    for r in (6, 7):
        buffer_ref[pl.ds(r, peers, stride=8), :] = jnp.zeros((peers, DK), f32)
    message_ref[...] = buffer_ref[...].astype(bf16)


def prefix_kernel(
    place_ref,
    arrived_ref,
    second_ref,
    out_ref,
    entry_ref,
    passed_ref,
    buffer_ref,
):
    passed_ref[...] = second_ref[...]
    place = place_ref[0]
    buffer_ref[...] = arrived_ref[...].astype(f32)
    peers = buffer_ref.shape[0] // 8
    vectors = buffer_ref[pl.ds(4, peers, stride=8), :]
    fact_rows = buffer_ref[pl.ds(5, peers, stride=8), :].T
    log_row = fact_rows[0:1, :] + fact_rows[1:2, :] + fact_rows[2:3, :]
    top_row = fact_rows[3:4, :] + fact_rows[4:5, :] + fact_rows[5:6, :]
    square = (peers, peers)
    i_id = row_ids(square)
    j_id = lane_ids(square)
    earlier = j_id < i_id
    before = jnp.where(earlier, log_row, 0.0)
    after = jnp.where(i_id > j_id, 1.0, 0.0).astype(f32)
    logs = jnp.dot(before, after, precision=highest, preferred_element_type=f32) + top_row
    logs = jnp.where(earlier, logs, lowest_log)
    top = jnp.max(logs, axis=1, keepdims=True)
    mix = jnp.where(earlier, jnp.exp(logs - top), 0.0)
    count = out_ref.shape[0] // peers
    for r in range(count):
        out_ref[pl.ds(r, peers, stride=count), :] = jnp.dot(
            mix,
            buffer_ref[pl.ds(r, peers, stride=8), :],
            precision=highest,
            preferred_element_type=f32,
        )
    entries = jnp.dot(mix, vectors, precision=highest, preferred_element_type=f32)
    mine = row_ids(entries.shape) == place
    vector = jnp.sum(jnp.where(mine, entries, 0.0), axis=0, keepdims=True)
    entry_top = jnp.sum(jnp.where(mine, top, 0.0), axis=0, keepdims=True)
    row = row_ids(entry_ref.shape)
    entry_ref[...] = jnp.where(row == 0, vector, jnp.where(row == 1, entry_top, 0.0))


def finish_kernel(
    head_ref,
    rows_ref,
    key_ref,
    value_ref,
    pair_ref,
    aux_ref,
    state_ref,
    entry_ref,
    gain_ref,
    first_ref,
    second_ref,
    out_ref,
):
    head = head_ref[0]
    width = out_ref.shape[1]
    query_low = projected(rows_ref, (first_ref, second_ref), 0, DK, width).astype(bf16)
    scores = lax.dot_general(
        query_low, key_ref[...], (((1,), (1,)), ((), ())), preferred_element_type=f32
    )
    weights = scores * pair_ref[...]
    numer = jnp.dot(weights.astype(bf16), value_ref[...], preferred_element_type=f32)
    denom = jnp.sum(weights, axis=1, keepdims=True)
    peers = 64
    count = state_ref.shape[0] // peers
    state = jnp.concatenate(
        [state_ref[pl.ds(r, peers, stride=count), :] for r in range(count)], axis=0
    )
    query = query_low.astype(f32)
    left = lax.dot_general(
        query, state, (((1,), (1,)), ((), ())), precision=highest, preferred_element_type=f32
    )
    entry_vec = entry_ref[0:1, :]
    entry_top = entry_ref[1:2, 0:1]
    left_denom = jnp.sum(query * entry_vec, axis=1, keepdims=True)
    aux = aux_ref[...]
    peak = column_of(aux, 1)
    carried = column_of(aux, 2) + entry_top
    top = jnp.maximum(peak, carried)
    own = jnp.exp(peak - top)
    old = jnp.exp(carried - top)
    numer = own * numer + old * left
    denom = own * denom + old * left_denom
    hidden = numer / jnp.maximum(jnp.abs(denom), jnp.exp(-top))
    gains = gain_ref[...].astype(f32)
    row = row_ids(gains.shape)
    gain = jnp.concatenate(
        [
            jnp.sum(jnp.where(row == 2 * head + k, gains, 0.0), axis=0, keepdims=True)
            for k in range(2)
        ],
        axis=1,
    )
    scale = lax.rsqrt(jnp.mean(hidden * hidden, axis=1, keepdims=True) + norm_floor)
    heads_out = (hidden * scale * gain).astype(bf16)
    for k in range(width // 256):
        out_ref[:, k * 256 : (k + 1) * 256] = lax.dot_general(
            heads_out,
            weight_rows((first_ref, second_ref), k, DK, DK + DV),
            (((1,), (1,)), ((), ())),
            preferred_element_type=f32,
        ).astype(bf16)


def on_device(
    tokens,
    pre_gain,
    w_query,
    w_key,
    w_value,
    w_igate,
    w_fgate,
    forget_bias,
    gate_drift,
    head_gain,
    w_out,
):
    rows, width = tokens.shape
    z_size, x_size = lax.axis_size("z"), lax.axis_size("x")
    peers = z_size * x_size
    core = lax.axis_index("c")
    head = (lax.axis_index("y") * 2 + core).astype(jnp.int32).reshape(1)
    place = (lax.axis_index("z") * x_size + lax.axis_index("x")).astype(jnp.int32).reshape(1)
    smem = pl.BlockSpec(memory_space=pltpu.SMEM)
    vmem = pl.BlockSpec(memory_space=pltpu.VMEM)
    limit = pltpu.CompilerParams(vmem_limit_bytes=24 * 2**20)

    own_rows = pl.pallas_call(
        prepare_kernel,
        out_shape=pltpu.VMEM((8, rows, width + 128), bf16),
        in_specs=[smem] + [vmem] * 5,
        out_specs=vmem,
        name="prepare",
    )(forget_bias, tokens, pre_gain.reshape(-1, 128), w_igate.T, w_fgate.T, gate_drift.T)
    all_rows = lax.all_to_all(own_rows, ("c", "y"), split_axis=0, concat_axis=0, tiled=True)
    all_rows = near(all_rows.reshape(-1, width + 128))
    length = all_rows.shape[0]

    pair = jnp.stack(
        [
            jnp.concatenate(
                [
                    w_key[:, c * DK : (c + 1) * DK],
                    w_value[:, c * DV : (c + 1) * DV],
                    w_query[:, c * DK : (c + 1) * DK],
                    w_out[:, c * DV : (c + 1) * DV],
                ],
                axis=1,
            )
            for c in range(2)
        ]
    )
    both = lax.all_gather(pair, "c", axis=0, tiled=False)
    mine = lax.dynamic_index_in_dim(both, core, axis=1, keepdims=False)
    mine = mine.reshape(-1, mine.shape[2])
    along_z = lax.all_gather(mine, "z", axis=0, tiled=True)
    cut = DK + DV

    rest = (along_z.shape[0], along_z.shape[1] - cut)
    pair_decay, aux, facts, copies, own_rest = pl.pallas_call(
        gates_kernel,
        out_shape=(
            pltpu.VMEM((length, length), f32),
            pltpu.VMEM((length, 128), f32),
            pltpu.VMEM((8, 128), f32),
            pltpu.VMEM((x_size, along_z.shape[0], cut), bf16),
            pltpu.VMEM(rest, bf16),
        ),
        in_specs=[smem, vmem, vmem],
        out_specs=(vmem,) * 5,
        compiler_params=limit,
        name="gates",
    )(head, all_rows, near(along_z))
    w_in = lax.all_to_all(copies, "x", split_axis=0, concat_axis=0, tiled=True)
    first, second = ((n, rest[1]) for n in (FIRST_ROWS, rest[0] - FIRST_ROWS))
    key, value, message, own_first, own_second = pl.pallas_call(
        state_kernel,
        out_shape=(
            pltpu.VMEM((length, DK), bf16),
            pltpu.VMEM((length, DV), bf16),
            pltpu.VMEM((peers * 8, DK), bf16),
            pltpu.VMEM(first, bf16),
            pltpu.VMEM(second, bf16),
        ),
        in_specs=[vmem] * 5,
        out_specs=(vmem,) * 5,
        scratch_shapes=[pltpu.VMEM((peers * 8, DK), f32)],
        compiler_params=limit,
        name="state",
    )(all_rows, near(w_in), aux, facts, own_rest)
    arrived = lax.all_to_all(message, ROWS, split_axis=0, concat_axis=0, tiled=True)
    first_part = near(lax.all_gather(own_first, "x", axis=0, tiled=False))
    slices, entry, own_second = pl.pallas_call(
        prefix_kernel,
        out_shape=(
            pltpu.VMEM((DV, DK), f32),
            jax.ShapeDtypeStruct((8, 128), f32),
            pltpu.VMEM(second, bf16),
        ),
        in_specs=[smem, vmem, vmem],
        out_specs=(vmem,) * 3,
        scratch_shapes=[pltpu.VMEM((peers * 8, DK), f32)],
        compiler_params=limit,
        name="prefix",
    )(place, near(arrived), own_second)
    state = lax.all_to_all(slices, ROWS, split_axis=0, concat_axis=0, tiled=True)
    second_part = near(lax.all_gather(own_second, "x", axis=0, tiled=False))
    partial = pl.pallas_call(
        finish_kernel,
        out_shape=pltpu.VMEM((length, width), bf16),
        in_specs=[smem] + [vmem] * 10,
        out_specs=vmem,
        compiler_params=limit,
        name="finish",
    )(
        head,
        all_rows,
        key,
        value,
        pair_decay,
        aux,
        near(state),
        entry,
        pltpu.with_memory_space_constraint(head_gain.reshape(-1, 128), pltpu.HBM),
        first_part,
        second_part,
    )
    halves = lax.all_to_all(
        partial.reshape(2, -1, width), "c", split_axis=0, concat_axis=0, tiled=True
    )
    joined = halves.astype(f32).sum(axis=0).astype(bf16)
    pieces = lax.all_to_all(
        joined.reshape(-1, rows, width), "y", split_axis=0, concat_axis=0, tiled=True
    )
    return pieces.astype(f32).sum(axis=0).astype(bf16)


def solution(mesh):
    split = Mesh(mesh.devices.reshape(16, 4, 2, mesh.shape["tp"]), ("z", "x", "c", "y"))
    return jax.shard_map(
        on_device,
        mesh=split,
        in_specs=(
            P(SP_TP, None),
            P(),
            P(SP, "y"),
            P(SP, "y"),
            P(SP, "y"),
            P(),
            P(),
            P(),
            P(SP, None),
            P(),
            P(SP, "y"),
        ),
        out_specs=P(SP_TP, None),
        check_vma=False,
    )
```
